32 devices in a mesh: ep: 8 (over z, y), tp: 4 (over x, core).
Axes of the slice: x: 2, y: 2, z: 4, core: 2. Of those that a mesh axis runs over, the one named last changes fastest.
Arguments:
- tokens: bfloat16 [16, 2048], P('ep'), may hold values from -6 to 6
- state_c: float32 [16, 8, 128, 256], P('ep', 'tp'), may hold values from -0.8 to 0.8
- state_n: float32 [16, 8, 128], P('ep', 'tp'), may hold values from -0.8 to 0.8
- state_m: float32 [16, 8], P('ep', 'tp'), may hold values from -2 to 2
- mix_gain: float32 [2048], replicated, may hold values from 0.1 to 1.9
- w_query: bfloat16 [2048, 1024], P('ep', 'tp'), may hold values from -0.125 to 0.125
- w_key: bfloat16 [2048, 1024], P('ep', 'tp'), may hold values from -0.125 to 0.125
- w_value: bfloat16 [2048, 2048], P('ep', 'tp'), may hold values from -0.125 to 0.125
- w_input_gate: bfloat16 [2048, 8], replicated, may hold values from -0.125 to 0.125
- w_forget_gate: bfloat16 [2048, 8], replicated, may hold values from -0.125 to 0.125
- forget_bias: float32 [8], replicated, may hold values from -1 to 4
- w_output: bfloat16 [2048, 2048], P('tp', 'ep'), may hold values from -0.125 to 0.125
- moe_gain: float32 [2048], replicated, may hold values from 0.1 to 1.9
- w_group: bfloat16 [2048, 4], replicated, may hold values from -0.25 to 0.25
- expert_ids: int32 [16, 2], P('ep'), may hold values from 0 to 7, all different within a row; in each aligned block of 2 rows (0 to 1, 2 to 3, ...) at most 1 rows name the same one
- expert_weight: float32 [16, 2], P('ep'), may hold values from 0.1 to 1
- w_exp_gate: bfloat16 [8, 2048, 512], P('ep', None, 'tp'), may hold values from -0.125 to 0.125
- w_exp_up: bfloat16 [8, 2048, 512], P('ep', None, 'tp'), may hold values from -0.25 to 0.25
- w_exp_down: bfloat16 [8, 512, 2048], P('ep', 'tp'), may hold values from -1 to 1
- w_dense: bfloat16 [2048, 2048], P('ep', 'tp'), may hold values from -0.125 to 0.125
- w_dense_gate: bfloat16 [2048], replicated, may hold values from -0.125 to 0.125
Outputs:
- mixed: bfloat16 [16, 2048], P('ep', 'tp')
- new_c: float32 [16, 8, 128, 256], P('ep', 'tp')
- new_n: float32 [16, 8, 128], P('ep', 'tp')
- new_m: float32 [16, 8], P('ep', 'tp')
The draws below stay inside these ranges and needn't reach their ends.
Inputs may be any that keep to these rules, and one draw needn't show every extreme that they name: `expert_ids`: each row names 2 different experts. In each aligned block of 2 rows (the rows of one index of ep) no expert is named by more than 1 row, a bound that some block reaches. Every expert is named by some row.
All inputs are finite; a program needn't handle non-finite values.
Results may differ from the reference program's by a relative error of at most 0.025.
Values may be sent and summed in bfloat16 or wider, within the bound.
No kernel may reach another device: no remote copies, remote signals or barrier semaphores. Data moves between devices by JAX's collectives and lax.ppermute only.
A program may use at most 64 MiB of HBM per device.

```python
import math
import jax
import jax.numpy as jnp
import numpy as np
from jax import lax

D = 2048
HEADS = 8
DQK = 128
DV = 256
FF = 512
GROUPS = 4
TOPK = 2
SEQ_DEV = 2
SEQS = 16
EXPERTS = 8
CAP = 1
N_TP = 4


def block_levels(own_key, shape, cuts, least, top_value):
    loudness, own = 1.0, jax.random.fold_in(own_key, 6)
    for dim, blocks in cuts:
        heights = jnp.exp(jax.random.uniform(jax.random.fold_in(own, dim), (blocks,), jnp.float32, least / len(cuts), top_value / len(cuts)))
        loudness = loudness * jnp.repeat(heights, shape[dim] // blocks).reshape([-1 if axis == dim else 1 for axis in range(len(shape))])
    return loudness


def assign_block(own_key, own, number, rows, count, top, reach, slope):
    order = jax.random.permutation(own_key, count)
    heavy_load, common = load_shares(count, rows * top, reach, slope, True), load_shares(count, rows * top, reach, slope, False)
    places = jnp.arange(count)

    def named(tallies, offset_by):
        used = int((tallies > 0).sum())
        fixed = max(1, used // 4)
        shifted = fixed + (places - fixed + offset_by * (used - fixed)) % max(1, count - fixed)
        return jnp.zeros((count,), jnp.int32).at[order[jnp.where(places < fixed, places, shifted)]].set(jnp.asarray(tallies, jnp.int32))

    tallies = jnp.where(number % 4 == 0, named(heavy_load, number // 4), named(common, number - number // 4 - 1))
    mixed = jax.random.permutation(jax.random.fold_in(own, 3), count)
    source_of, taker = mixed[0:count // 2 * 2:2], mixed[1:count // 2 * 2:2]
    slack = jnp.minimum(tallies[source_of] - 1, reach - tallies[taker]) // 2
    slack = jnp.where((source_of == order[0]) | (taker == order[0]) | (tallies[taker] == 0), 0, jnp.maximum(slack, 0))
    shifted = jax.random.randint(jax.random.fold_in(own, 4), (count // 2,), 0, 1 << 20) % (slack + 1)
    tallies = tallies.at[source_of].add(-shifted).at[taker].add(shifted)
    members = jnp.searchsorted(jnp.cumsum(tallies), jnp.arange(rows * top), side="right").astype(jnp.int32)
    listing = members.reshape(top, rows).T
    listing = listing[jax.random.permutation(jax.random.fold_in(own, 1), rows)]
    offset_by = jax.random.randint(jax.random.fold_in(own, 2), (rows, 1), 0, top)
    return jnp.take_along_axis(listing, (jnp.arange(top)[None, :] + offset_by) % top, axis=1)


def load_shares(count, total, reach, slope, full):
    portions = [(1 << 20) // math.isqrt(grade ** slope) + 1 for grade in range(1, count + 1)]
    largest = reach if full else min(reach, max(-(-total // count), total * portions[0] // sum(portions)))
    least = 1 if total - largest >= count - 1 else 0
    counts, spare = [largest] + [least] * (count - 1), total - largest - least * (count - 1)
    while spare > 0:
        candidates = [i for i in range(1, count) if counts[i] < largest] or [i for i in range(1, count) if counts[i] < reach]
        whole, left = sum([portions[i] for i in candidates]), spare
        for i in candidates:
            more = min(reach - counts[i], max(1, left * portions[i] // whole), spare)
            counts[i] = counts[i] + more
            spare = spare - more
    return np.array(counts)


def gaussian(own_key, dims, scale, limit, shards=(), kind=jnp.bfloat16):
    result = scale * jax.random.normal(own_key, dims, jnp.float32)
    if shards:
        result = result * block_levels(own_key, dims, shards, -0.22, 0.18)
    return jnp.clip(result, -limit, limit).astype(kind)


def setup_inputs(seed: int = 0) -> dict:
    splits = jax.random.split(jax.random.key(seed), 22)
    tokens = gaussian(splits[0], (SEQS, D), 1.0, 6.0, ((0, 8),))
    state_c = gaussian(splits[1], (SEQS, HEADS, DQK, DV), 0.1, 0.8, ((0, 8), (1, 4)), jnp.float32)
    state_n = gaussian(splits[2], (SEQS, HEADS, DQK), 0.1, 0.8, ((0, 8), (1, 4)), jnp.float32)
    state_m = jnp.clip(jax.random.uniform(splits[3], (SEQS, HEADS), jnp.float32, -2.0, 2.0) * block_levels(splits[3], (SEQS, HEADS), ((0, 8), (1, 4)), -0.4, 0.0), -2.0, 2.0)
    mix_gain = jnp.clip(1.0 + 0.18 * jax.random.normal(splits[4], (D,), jnp.float32), 0.1, 1.9)
    w_query = gaussian(splits[5], (D, HEADS * DQK), D ** -0.5, 0.125, ((0, 8), (1, 4)))
    w_key = gaussian(splits[6], (D, HEADS * DQK), D ** -0.5, 0.125, ((0, 8), (1, 4)))
    w_value = gaussian(splits[7], (D, HEADS * DV), D ** -0.5, 0.125, ((0, 8), (1, 4)))
    w_input_gate = gaussian(splits[8], (D, HEADS), D ** -0.5, 0.125)
    w_forget_gate = gaussian(splits[9], (D, HEADS), D ** -0.5, 0.125)
    forget_bias = jnp.clip(jax.random.uniform(splits[10], (HEADS,), jnp.float32, -1.0, 4.0), -1.0, 4.0)
    w_output = gaussian(splits[11], (HEADS * DV, D), (HEADS * DV) ** -0.5, 0.125, ((0, 4), (1, 8)))
    moe_gain = jnp.clip(1.0 + 0.18 * jax.random.normal(splits[12], (D,), jnp.float32), 0.1, 1.9)
    w_group = gaussian(splits[13], (D, GROUPS), (D // 4) ** -0.5, 0.25)
    expert_ids_keys = jax.random.split(jax.random.fold_in(splits[14], 1), SEQS // SEQ_DEV)
    expert_ids_turns = jax.random.permutation(jax.random.fold_in(splits[14], 3), SEQS // SEQ_DEV)
    expert_ids = jax.vmap(lambda own, number: assign_block(jax.random.fold_in(splits[14], 2), own, number, SEQ_DEV, EXPERTS, TOPK, CAP, 2))(expert_ids_keys, expert_ids_turns).reshape((SEQS, TOPK))
    expert_weight = jnp.clip(jnp.exp(math.log(1.0) - 2.3025851 * jax.random.uniform(splits[15], (SEQS, TOPK), jnp.float32) ** block_levels(splits[15], (SEQS, TOPK), ((0, 8),), -0.2, 0.2)), 0.1, 1.0)
    w_exp_gate = gaussian(splits[16], (EXPERTS, D, FF), D ** -0.5, 0.125, ((0, 8), (2, 4)))
    w_exp_up = gaussian(splits[17], (EXPERTS, D, FF), (D // 4) ** -0.5, 0.25, ((0, 8), (2, 4)))
    w_exp_down = gaussian(splits[18], (EXPERTS, FF, D), (FF // 16) ** -0.5, 1.0, ((0, 8), (1, 4)))
    w_dense = gaussian(splits[19], (D, D), D ** -0.5, 0.125, ((0, 8), (1, 4)))
    w_dense_gate = gaussian(splits[20], (D,), D ** -0.5, 0.125)
    return dict(tokens=tokens, state_c=state_c, state_n=state_n, state_m=state_m, mix_gain=mix_gain, w_query=w_query, w_key=w_key, w_value=w_value, w_input_gate=w_input_gate, w_forget_gate=w_forget_gate, forget_bias=forget_bias, w_output=w_output, moe_gain=moe_gain, w_group=w_group, expert_ids=expert_ids, expert_weight=expert_weight, w_exp_gate=w_exp_gate, w_exp_up=w_exp_up, w_exp_down=w_exp_down, w_dense=w_dense, w_dense_gate=w_dense_gate)


eps = 1e-06

def rms_norm(values, gain):
    widened = values.astype(jnp.float32)
    inverse = lax.rsqrt(lax.optimization_barrier(jnp.mean(widened * widened, axis=-1, keepdims=True)) + eps)
    return (widened * inverse * gain).astype(jnp.bfloat16)

def rounded(values):
    return lax.optimization_barrier(values.astype(jnp.bfloat16)).astype(jnp.float32)

def memory_step(query_rows, key_rows, value_rows, in_gate, forget, state_c, state_n, state_m):
    seq_count, head_count = state_m.shape
    q_heads = query_rows.reshape(seq_count, head_count, -1)
    k_heads = key_rows.reshape(seq_count, head_count, -1) * q_heads.shape[-1] ** (-0.5)
    v_heads = value_rows.reshape(seq_count, head_count, -1)
    new_m = jnp.maximum(forget + state_m, in_gate)
    decay = jnp.exp(forget + state_m - new_m)
    inflow = jnp.exp(in_gate - new_m)
    new_c = decay[..., None, None] * state_c + (inflow[..., None] * k_heads)[..., :, None] * v_heads[..., None, :]
    new_n = decay[..., None] * state_n + inflow[..., None] * k_heads
    numer = jnp.einsum('shd,shde->she', q_heads, new_c, precision=lax.Precision.HIGHEST)
    denom = jnp.maximum(jnp.abs(lax.optimization_barrier(jnp.sum(q_heads * new_n, axis=-1))), 1.0)
    heads = (numer / denom[..., None]).astype(jnp.bfloat16).reshape(seq_count, -1)
    return (heads, new_c, new_n, new_m)

def reference(tokens, state_c, state_n, state_m, mix_gain, w_query, w_key, w_value, w_input_gate, w_forget_gate, forget_bias, w_output, moe_gain, w_group, expert_ids, expert_weight, w_exp_gate, w_exp_up, w_exp_down, w_dense, w_dense_gate):
    seq_count = tokens.shape[0]
    normed = rms_norm(tokens, mix_gain)
    query_rows = rounded(jnp.dot(normed, w_query, preferred_element_type=jnp.float32))
    key_rows = rounded(jnp.dot(normed, w_key, preferred_element_type=jnp.float32))
    value_rows = rounded(jnp.dot(normed, w_value, preferred_element_type=jnp.float32))
    in_gate = jnp.dot(normed, w_input_gate, preferred_element_type=jnp.float32)
    forget = jax.nn.log_sigmoid(jnp.dot(normed, w_forget_gate, preferred_element_type=jnp.float32) + forget_bias)
    heads, new_c, new_n, new_m = memory_step(query_rows, key_rows, value_rows, in_gate, forget, state_c, state_n, state_m)
    head_blocks = heads.reshape(seq_count, N_TP, -1).astype(jnp.float32)
    out_blocks = w_output.reshape(N_TP, -1, D).astype(jnp.float32)
    partials = rounded(jnp.einsum('stf,tfd->tsd', head_blocks, out_blocks))
    residual = (tokens.astype(jnp.float32) + lax.optimization_barrier(jnp.sum(partials, axis=0))).astype(jnp.bfloat16)
    normed2 = rms_norm(residual, moe_gain)
    group_prob = jax.nn.softmax(jnp.dot(normed2, w_group, preferred_element_type=jnp.float32), axis=-1)
    per_group = EXPERTS // GROUPS
    member = (expert_ids // per_group)[..., None] == jnp.arange(GROUPS, dtype=jnp.int32)[None, None, :]
    picked = lax.optimization_barrier(jnp.sum(jnp.where(member, group_prob[:, None, :], 0.0), axis=-1))
    route = picked * expert_weight / lax.optimization_barrier(jnp.sum(expert_weight, axis=1, keepdims=True))
    flat_ids = expert_ids.reshape(-1).astype(jnp.int32)
    repeated = jnp.repeat(normed2, TOPK, axis=0)

    def run_one(item):
        ident, token_row = item
        gate_matrix = lax.dynamic_index_in_dim(w_exp_gate, ident, 0, keepdims=False)
        up_matrix = lax.dynamic_index_in_dim(w_exp_up, ident, 0, keepdims=False)
        down_matrix = lax.dynamic_index_in_dim(w_exp_down, ident, 0, keepdims=False)
        gate_act = jnp.dot(token_row[None, :], gate_matrix, preferred_element_type=jnp.float32)
        up_act = jnp.dot(token_row[None, :], up_matrix, preferred_element_type=jnp.float32)
        hidden = (jax.nn.silu(gate_act) * up_act).astype(jnp.bfloat16)
        hidden_blocks = hidden.reshape(N_TP, -1).astype(jnp.float32)
        down_blocks = down_matrix.reshape(N_TP, -1, D).astype(jnp.float32)
        parts = rounded(jnp.einsum('tf,tfd->td', hidden_blocks, down_blocks))
        return lax.optimization_barrier(jnp.sum(parts, axis=0)).astype(jnp.bfloat16)
    expert_out = lax.map(run_one, (flat_ids, repeated))
    moe = lax.optimization_barrier(jnp.sum(route[..., None] * expert_out.astype(jnp.float32).reshape(seq_count, TOPK, D), axis=1))
    dense_gate = jax.nn.sigmoid(jnp.dot(normed2, w_dense_gate, preferred_element_type=jnp.float32))
    dense = dense_gate[:, None] * jnp.dot(normed2, w_dense, preferred_element_type=jnp.float32)
    mixed = (residual.astype(jnp.float32) + moe + dense).astype(jnp.bfloat16)
    return (mixed, new_c, new_n, new_m)
```

```python
import jax
import jax.numpy as jnp
from jax import lax
from jax.sharding import PartitionSpec as P

eps = 1e-06
BOTH = ("ep", "tp")


def exchange(chunks, axes):
    return lax.all_to_all(chunks, axes, split_axis=0, concat_axis=0, tiled=True)


def rms_norm(values, gain):
    widened = values.astype(jnp.float32)
    inverse = lax.rsqrt(jnp.mean(widened * widened, axis=-1, keepdims=True) + eps)
    return (widened * inverse * gain).astype(jnp.bfloat16)


def per_device(
    tokens,
    state_c,
    state_n,
    state_m,
    mix_gain,
    w_query,
    w_key,
    w_value,
    w_input_gate,
    w_forget_gate,
    forget_bias,
    w_output,
    moe_gain,
    w_group,
    expert_ids,
    expert_weight,
    w_exp_gate,
    w_exp_up,
    w_exp_down,
    w_dense,
    w_dense_gate,
):
    f32, bf16 = jnp.float32, jnp.bfloat16
    own, width = tokens.shape
    tp_count = lax.axis_size("tp")
    ep_count = lax.axis_size("ep")
    tp_rank = lax.axis_index("tp")
    ep_rank = lax.axis_index("ep")
    seqs = own * ep_count
    head_count = state_m.shape[1]
    rows = w_query.shape[0]
    qk_cols = w_query.shape[1]
    share = width // tp_count
    cols = w_output.shape[1]
    experts_here = w_exp_gate.shape[0]
    expert_count = experts_here * ep_count

    spread = exchange(tokens.reshape(own, ep_count, rows).transpose(1, 0, 2), "ep")
    spread = spread.reshape(seqs, rows)
    gain_rows = lax.dynamic_slice_in_dim(mix_gain, ep_rank * rows, rows)
    scaled = (spread.astype(f32) * gain_rows).astype(bf16)
    sums = [jnp.dot(scaled, w, preferred_element_type=f32) for w in (w_query, w_key, w_value)]
    expert_of = jnp.arange(expert_count, dtype=jnp.int32)
    shares = expert_weight / jnp.sum(expert_weight, axis=1, keepdims=True)
    picks = jnp.sum(
        jnp.where(expert_ids[None, :, :] == expert_of[:, None, None], shares[None], 0.0), axis=2
    )
    picks = picks.reshape(ep_count, experts_here, own).transpose(0, 2, 1)
    picks = jnp.pad(picks, ((0, 0), (0, 0), (0, -experts_here % 128))).reshape(seqs, -1)
    parts = exchange(jnp.concatenate(sums + [picks], axis=1).reshape(ep_count, own, -1), "ep")
    wide = tokens.astype(f32)
    inverse = lax.rsqrt(jnp.mean(wide * wide, axis=-1, keepdims=True) + eps)
    normed = (wide * inverse * mix_gain).astype(bf16)
    packed = 2 * qk_cols + w_value.shape[1]
    coef = parts[:, :, packed : packed + experts_here].reshape(seqs, experts_here)
    qkv = (jnp.sum(parts[:, :, :packed], axis=0) * inverse).astype(bf16).astype(f32)
    gate_all = jnp.dot(normed, w_input_gate, preferred_element_type=f32)
    forget_all = jax.nn.log_sigmoid(
        jnp.dot(normed, w_forget_gate, preferred_element_type=f32) + forget_bias
    )
    in_gate = lax.dynamic_slice_in_dim(gate_all, tp_rank * head_count, head_count, 1)
    forget = lax.dynamic_slice_in_dim(forget_all, tp_rank * head_count, head_count, 1)
    q_heads = qkv[:, :qk_cols].reshape(own, head_count, -1)
    k_heads = qkv[:, qk_cols : 2 * qk_cols].reshape(own, head_count, -1)
    k_heads = k_heads * q_heads.shape[-1] ** (-0.5)
    v_heads = qkv[:, 2 * qk_cols :].reshape(own, head_count, -1)
    new_m = jnp.maximum(forget + state_m, in_gate)
    decay = jnp.exp(forget + state_m - new_m)
    inflow = jnp.exp(in_gate - new_m)
    new_c = (
        decay[..., None, None] * state_c
        + (inflow[..., None] * k_heads)[..., :, None] * v_heads[..., None, :]
    )
    new_n = decay[..., None] * state_n + inflow[..., None] * k_heads
    recalled = jnp.sum(q_heads[..., None] * state_c, axis=2)
    match = jnp.sum(q_heads * k_heads, axis=-1)
    numer = decay[..., None] * recalled + (inflow * match)[..., None] * v_heads
    denom = jnp.maximum(jnp.abs(jnp.sum(q_heads * new_n, axis=-1)), 1.0)
    heads = (numer / denom[..., None]).astype(bf16).reshape(own, -1)
    heads_all = exchange(jnp.broadcast_to(heads[None], (ep_count,) + heads.shape), "ep")
    out_part = jnp.dot(heads_all.reshape(seqs, -1), w_output, preferred_element_type=f32)
    out_part = (out_part + spread.astype(f32) * (1.0 / tp_count)).astype(bf16)
    every = exchange(jnp.broadcast_to(out_part[None], (ep_count * tp_count,) + out_part.shape), BOTH)
    residual = jnp.sum(every.reshape(ep_count, tp_count, seqs, cols).astype(f32), axis=1)
    residual = residual.astype(bf16).transpose(1, 0, 2).reshape(seqs, width)
    normed2 = rms_norm(residual, moe_gain)
    group_count = w_group.shape[1]
    group_prob = jax.nn.softmax(jnp.dot(normed2, w_group, preferred_element_type=f32), axis=-1)
    group_of = (ep_rank * experts_here + jnp.arange(experts_here, dtype=jnp.int32)) // (
        expert_count // group_count
    )
    member = group_of[:, None] == jnp.arange(group_count, dtype=jnp.int32)[None, :]
    chance = jnp.sum(jnp.where(member[None], group_prob[:, None, :], 0.0), axis=-1)
    route = chance * coef
    total = jnp.zeros((seqs, width), f32)
    for x in range(experts_here):
        gate_act = jnp.dot(normed2, w_exp_gate[x], preferred_element_type=f32)
        up_act = jnp.dot(normed2, w_exp_up[x], preferred_element_type=f32)
        hidden = (jax.nn.silu(gate_act) * up_act).astype(bf16)
        total += route[:, x : x + 1] * jnp.dot(hidden, w_exp_down[x], preferred_element_type=f32)
    dense_gate = jax.nn.sigmoid(jnp.dot(normed2, w_dense_gate, preferred_element_type=f32))
    dense_in = lax.dynamic_slice_in_dim(normed2, ep_rank * rows, rows, 1)
    dense = dense_gate[:, None] * jnp.dot(dense_in, w_dense, preferred_element_type=f32)
    total = total.reshape(seqs, tp_count, share)
    mine = jnp.arange(tp_count, dtype=jnp.int32) == tp_rank
    total = (total + jnp.where(mine[None, :, None], dense[:, None, :], 0.0)).astype(bf16)
    total = total.reshape(ep_count, own, tp_count, share).transpose(0, 2, 1, 3)
    last = exchange(total.reshape(ep_count * tp_count, own, share), BOTH)
    own_rows = lax.dynamic_slice(residual, (ep_rank * own, tp_rank * share), (own, share))
    mixed = (own_rows.astype(f32) + jnp.sum(last.astype(f32), axis=0)).astype(bf16)
    return (mixed, new_c, new_n, new_m)


def solution(mesh):
    placed = (
        P("ep", None),
        P("ep", "tp", None, None),
        P("ep", "tp", None),
        P("ep", "tp"),
        P(),
        P("ep", "tp"),
        P("ep", "tp"),
        P("ep", "tp"),
        P(),
        P(),
        P(),
        P("tp", "ep"),
        P(),
        P(),
        P("ep", None),
        P("ep", None),
        P("ep", None, "tp"),
        P("ep", None, "tp"),
        P("ep", "tp", None),
        P("ep", "tp"),
        P(),
    )
    return jax.shard_map(
        per_device,
        mesh=mesh,
        in_specs=placed,
        out_specs=(P("ep", "tp"), P("ep", "tp", None, None), P("ep", "tp", None), P("ep", "tp")),
        check_vma=False,
    )
```

```python
import functools

import jax
import jax.numpy as jnp
from jax import lax
from jax.experimental import pallas as pl
from jax.experimental.pallas import tpu as pltpu
from jax.sharding import PartitionSpec as P

eps = 1e-06
BOTH = ("ep", "tp")
f32, bf16 = jnp.float32, jnp.bfloat16
VMEM_BYTES = 12 << 20


def exchange(chunks, axes):
    return lax.all_to_all(chunks, axes, split_axis=0, concat_axis=0, tiled=True)


def shaped(*dims, dtype=f32):
    return jax.ShapeDtypeStruct(dims, dtype)


def run(body, outs, name, scalars, *arrays):
    specs = [pl.BlockSpec(memory_space=pltpu.SMEM)] * len(scalars)
    specs += [pl.BlockSpec(memory_space=pltpu.VMEM)] * len(arrays)
    return pl.pallas_call(
        body,
        out_shape=outs,
        in_specs=specs,
        name=name,
        compiler_params=pltpu.CompilerParams(vmem_limit_bytes=VMEM_BYTES),
    )(*scalars, *arrays)


def dot(left, right, dims=((1,), (0,))):
    return lax.dot_general(left, right, (dims, ((), ())), preferred_element_type=f32)


def project_body(spread, gain, w_query, w_key, w_value, picks, out):
    scaled = (spread[...].astype(f32) * gain[...]).astype(bf16)
    at, own = 0, out.shape[1]
    for w in (w_query, w_key, w_value):
        sums = dot(scaled, w[...])
        for b in range(out.shape[0]):
            out[b, :, at : at + w.shape[1]] = sums[b * own : (b + 1) * own]
        at += w.shape[1]
    for b in range(out.shape[0]):
        out[b, :, at:] = picks[b]


def memory_body(parts, inverse, decay, inflow, state_c, kept_n, heads_out, new_n_out, qkv_out, coef_out):
    blocks, own, _ = parts.shape
    head_count, dqk, dv = state_c.shape[1:]
    packed = head_count * (2 * dqk + dv)
    total = parts[0, :, :packed]
    for b in range(1, blocks):
        total += parts[b, :, :packed]
    for b in range(blocks):
        coef_out[b * own : (b + 1) * own, :] = parts[b, :, packed:]
    qkv = (total * inverse[...]).astype(bf16).astype(f32)
    qkv_out[...] = qkv
    for i in range(own):
        for h in range(head_count):
            q = qkv[i : i + 1, h * dqk : (h + 1) * dqk]
            at = (head_count + h) * dqk
            k = qkv[i : i + 1, at : at + dqk] * dqk ** (-0.5)
            at = 2 * head_count * dqk + h * dv
            v = qkv[i : i + 1, at : at + dv]
            kept, flow = decay[i : i + 1, h : h + 1], inflow[i : i + 1, h : h + 1]
            new_n = kept_n[i, h : h + 1, :] + flow * k
            new_n_out[i, h : h + 1, :] = new_n
            recalled = lax.dot_general(
                q, state_c[i, h], (((1,), (0,)), ((), ())),
                preferred_element_type=f32, precision=lax.Precision.HIGHEST,
            )
            numer = kept * recalled + (flow * jnp.sum(q * k, axis=1, keepdims=True)) * v
            denom = jnp.maximum(jnp.abs(jnp.sum(q * new_n, axis=1, keepdims=True)), 1.0)
            head = (numer / denom).astype(bf16)
            for d in range(heads_out.shape[0]):
                heads_out[d, i : i + 1, h * dv : (h + 1) * dv] = head


def output_body(tp_ref, heads, near, far, spread, out):
    own = heads.shape[1]
    tp_count = heads.shape[0] * own // spread.shape[0]
    half, some = out.shape[2], out.shape[1]
    rank = tp_ref[0]
    side, part = rank % 2, rank // 2
    blocks = some // own
    at = pl.ds(pl.multiple_of(side * half, 128), half)
    tokens = spread[:, at].astype(f32)
    total = jnp.where(part == 0, tokens[:some], tokens[some:])
    for d in range(tp_count):
        source = rank ^ d
        pieces = [heads[(part * blocks + b) * tp_count + source].astype(f32) for b in range(blocks)]
        left = jnp.concatenate(pieces, axis=0).astype(bf16)
        total += dot(left, (far if d // 2 else near)[d % 2])
    total = total.astype(bf16)
    for d in range(out.shape[0]):
        out[d] = total


def experts_body(
    ranks, every, coef, gain, w_group, w_dense_gate, w_gate, w_up, w_down, w_dense,
    out, own_out, normed_buf, total_buf, *, per_group, ep_count,
):
    seqs, width = normed_buf.shape
    count, some, half = every.shape
    tp_count = count // ep_count
    own, share = out.shape[1], out.shape[2]
    ep_rank, tp_rank = ranks[0], ranks[1]
    halves = []
    for part in range(2):
        tiles = [every[e * tp_count + part * 2 + s].astype(f32) for e in range(ep_count) for s in range(2)]
        halves.append(jnp.concatenate(tiles, axis=1))
    residual = jnp.concatenate(halves, axis=0)
    inverse = lax.rsqrt(jnp.mean(residual * residual, axis=-1, keepdims=True) + eps)
    normed = (residual * inverse * gain[...]).astype(bf16)
    normed_buf[...] = normed.astype(f32)
    total_buf[...] = residual
    columns = pl.ds(pl.multiple_of(tp_rank * share, 128), share)
    mine = total_buf[:, columns]
    row = lax.broadcasted_iota(jnp.int32, mine.shape, 0)
    for i in range(own):
        held = jnp.where(row == ep_rank * own + i, mine, 0.0)
        own_out[i : i + 1, :] = jnp.sum(held, axis=0, keepdims=True)
    logits = dot(normed, w_group[...], ((1,), (1,)))
    powers = jnp.exp(logits - jnp.max(logits, axis=1, keepdims=True))
    lane = lax.broadcasted_iota(jnp.int32, logits.shape, 1)
    chosen = jnp.sum(jnp.where(lane == ep_rank // per_group, powers, 0.0), axis=1, keepdims=True)
    route = chosen / jnp.sum(powers, axis=1, keepdims=True) * coef[:, 0:1]
    gate_act = dot(normed, w_gate[0])
    up_act = dot(normed, w_up[0])
    hidden = (gate_act * jax.nn.sigmoid(gate_act) * up_act).astype(bf16)
    total_buf[...] = route * dot(hidden, w_down[0])
    rows = w_dense.shape[0]
    some_in = normed_buf[:, pl.ds(pl.multiple_of(ep_rank * rows, 128), rows)].astype(bf16)
    gate = jnp.sum(normed.astype(f32) * w_dense_gate[...].astype(f32), axis=1, keepdims=True)
    total_buf[:, columns] += jax.nn.sigmoid(gate) * dot(some_in, w_dense[...])
    for b in range(ep_count):
        for t in range(tp_count):
            piece = total_buf[b * own : (b + 1) * own, t * share : (t + 1) * share]
            out[b * tp_count + t] = piece.astype(bf16)


def fast_device(
    tokens, state_c, state_n, state_m, mix_gain, w_query, w_key, w_value, w_input_gate, w_forget_gate,
    forget_bias, w_output, moe_gain, w_group, expert_ids, expert_weight, w_exp_gate, w_exp_up,
    w_exp_down, w_dense, w_dense_gate,
):
    own, width = tokens.shape
    tp_count, ep_count = lax.axis_size("tp"), lax.axis_size("ep")
    tp_rank, ep_rank = lax.axis_index("tp"), lax.axis_index("ep")
    every_count = ep_count * tp_count
    seqs, (rows, qk_cols), v_cols = own * ep_count, w_query.shape, w_value.shape[1]
    head_count, share, half = state_m.shape[1], width // tp_count, w_output.shape[1] // 2
    tp_ref, ranks = tp_rank.reshape(1), jnp.stack([ep_rank, tp_rank])
    gain = mix_gain.reshape(1, width)
    packed = 2 * qk_cols + v_cols
    with jax.named_scope("r1"):
        spread = exchange(tokens.reshape(own, ep_count, rows).transpose(1, 0, 2), "ep")
    spread = spread.reshape(seqs, rows)
    side = tp_rank % 2
    with jax.named_scope("swap"):
        given = lax.dynamic_slice_in_dim(w_output, (1 - side) * half, half, 1)
        taken = lax.ppermute(given, "tp", [(d, d ^ 1) for d in range(tp_count)])
    with jax.named_scope("cross"):
        pair = jnp.stack([lax.dynamic_slice_in_dim(w_output, side * half, half, 1), taken])
        far = lax.ppermute(pair, "tp", [(d, d ^ 2) for d in range(tp_count)])
    gain_rows = lax.dynamic_slice_in_dim(gain, ep_rank * rows, rows, 1)
    expert_of = jnp.arange(ep_count, dtype=jnp.int32)
    shares = expert_weight / jnp.sum(expert_weight, axis=1, keepdims=True)
    picks = jnp.where(expert_ids[None, :, :] == expert_of[:, None, None], shares[None], 0.0)
    picks = jnp.broadcast_to(jnp.sum(picks, axis=2)[..., None], (ep_count, own, 128))
    wide = tokens.astype(f32)
    inverse = lax.rsqrt(jnp.mean(wide * wide, axis=-1, keepdims=True) + eps)
    normed = (wide * inverse * mix_gain).astype(bf16)
    gate_all = jnp.dot(normed, w_input_gate, preferred_element_type=f32)
    forget_all = jax.nn.log_sigmoid(
        jnp.dot(normed, w_forget_gate, preferred_element_type=f32) + forget_bias
    )
    in_gate = lax.dynamic_slice_in_dim(gate_all, tp_rank * head_count, head_count, 1)
    forget = lax.dynamic_slice_in_dim(forget_all, tp_rank * head_count, head_count, 1)
    new_m = jnp.maximum(forget + state_m, in_gate)
    decay = jnp.exp(forget + state_m - new_m)
    inflow = jnp.exp(in_gate - new_m)
    kept_n = decay[..., None] * state_n
    sums = run(
        project_body, shaped(ep_count, own, packed + 128), "project", (),
        spread, gain_rows, w_query, w_key, w_value, picks,
    )
    with jax.named_scope("r2"):
        parts = exchange(sums, "ep")
    heads, new_n, qkv, coef = run(
        memory_body,
        (
            shaped(every_count, own, v_cols, dtype=bf16), shaped(*state_n.shape),
            shaped(own, packed), shaped(seqs, 128),
        ),
        "memory", (), parts, inverse, decay, inflow, state_c, kept_n,
    )
    with jax.named_scope("r3"):
        heads = exchange(heads, BOTH)
    k_heads = qkv[:, qk_cols : 2 * qk_cols].reshape(own, head_count, -1)
    k_heads = k_heads * k_heads.shape[-1] ** (-0.5)
    v_heads = qkv[:, 2 * qk_cols :].reshape(own, head_count, -1)
    new_c = (
        decay[..., None, None] * state_c
        + (inflow[..., None] * k_heads)[..., :, None] * v_heads[..., None, :]
    )
    out = run(
        output_body, shaped(every_count, seqs // 2, half, dtype=bf16), "output", (tp_ref,),
        heads, pair, far, spread,
    )
    with jax.named_scope("r4"):
        every = exchange(out, BOTH)
    last, own_rows = pl.pallas_call(
        functools.partial(
            experts_body, per_group=ep_count // w_group.shape[1], ep_count=ep_count
        ),
        out_shape=(shaped(every_count, own, share, dtype=bf16), shaped(own, share)),
        in_specs=[pl.BlockSpec(memory_space=pltpu.SMEM)] + [pl.BlockSpec(memory_space=pltpu.VMEM)] * 9,
        scratch_shapes=[pltpu.VMEM((seqs, width), f32)] * 2,
        name="experts",
        compiler_params=pltpu.CompilerParams(vmem_limit_bytes=VMEM_BYTES),
    )(
        ranks, every, coef, moe_gain.reshape(1, width), w_group.T, w_dense_gate.reshape(1, width),
        w_exp_gate, w_exp_up, w_exp_down, w_dense,
    )
    with jax.named_scope("r5"):
        last = exchange(last, BOTH)
    mixed = (own_rows + jnp.sum(last.astype(f32), axis=0)).astype(bf16)
    return (mixed, new_c, new_n, new_m)


def rms_norm(values, gain):
    widened = values.astype(jnp.float32)
    inverse = lax.rsqrt(jnp.mean(widened * widened, axis=-1, keepdims=True) + eps)
    return (widened * inverse * gain).astype(jnp.bfloat16)


def plain_device(
    tokens,
    state_c,
    state_n,
    state_m,
    mix_gain,
    w_query,
    w_key,
    w_value,
    w_input_gate,
    w_forget_gate,
    forget_bias,
    w_output,
    moe_gain,
    w_group,
    expert_ids,
    expert_weight,
    w_exp_gate,
    w_exp_up,
    w_exp_down,
    w_dense,
    w_dense_gate,
):
    own, width = tokens.shape
    tp_count = lax.axis_size("tp")
    ep_count = lax.axis_size("ep")
    tp_rank = lax.axis_index("tp")
    ep_rank = lax.axis_index("ep")
    seqs = own * ep_count
    head_count = state_m.shape[1]
    rows = w_query.shape[0]
    qk_cols = w_query.shape[1]
    share = width // tp_count
    cols = w_output.shape[1]
    experts_here = w_exp_gate.shape[0]
    expert_count = experts_here * ep_count

    spread = exchange(tokens.reshape(own, ep_count, rows).transpose(1, 0, 2), "ep")
    spread = spread.reshape(seqs, rows)
    gain_rows = lax.dynamic_slice_in_dim(mix_gain, ep_rank * rows, rows)
    scaled = (spread.astype(f32) * gain_rows).astype(bf16)
    sums = [jnp.dot(scaled, w, preferred_element_type=f32) for w in (w_query, w_key, w_value)]
    expert_of = jnp.arange(expert_count, dtype=jnp.int32)
    shares = expert_weight / jnp.sum(expert_weight, axis=1, keepdims=True)
    picks = jnp.sum(
        jnp.where(expert_ids[None, :, :] == expert_of[:, None, None], shares[None], 0.0), axis=2
    )
    picks = picks.reshape(ep_count, experts_here, own).transpose(0, 2, 1)
    picks = jnp.pad(picks, ((0, 0), (0, 0), (0, -experts_here % 128))).reshape(seqs, -1)
    parts = exchange(jnp.concatenate(sums + [picks], axis=1).reshape(ep_count, own, -1), "ep")
    wide = tokens.astype(f32)
    inverse = lax.rsqrt(jnp.mean(wide * wide, axis=-1, keepdims=True) + eps)
    normed = (wide * inverse * mix_gain).astype(bf16)
    packed = 2 * qk_cols + w_value.shape[1]
    coef = parts[:, :, packed : packed + experts_here].reshape(seqs, experts_here)
    qkv = (jnp.sum(parts[:, :, :packed], axis=0) * inverse).astype(bf16).astype(f32)
    gate_all = jnp.dot(normed, w_input_gate, preferred_element_type=f32)
    forget_all = jax.nn.log_sigmoid(
        jnp.dot(normed, w_forget_gate, preferred_element_type=f32) + forget_bias
    )
    in_gate = lax.dynamic_slice_in_dim(gate_all, tp_rank * head_count, head_count, 1)
    forget = lax.dynamic_slice_in_dim(forget_all, tp_rank * head_count, head_count, 1)
    q_heads = qkv[:, :qk_cols].reshape(own, head_count, -1)
    k_heads = qkv[:, qk_cols : 2 * qk_cols].reshape(own, head_count, -1)
    k_heads = k_heads * q_heads.shape[-1] ** (-0.5)
    v_heads = qkv[:, 2 * qk_cols :].reshape(own, head_count, -1)
    new_m = jnp.maximum(forget + state_m, in_gate)
    decay = jnp.exp(forget + state_m - new_m)
    inflow = jnp.exp(in_gate - new_m)
    new_c = (
        decay[..., None, None] * state_c
        + (inflow[..., None] * k_heads)[..., :, None] * v_heads[..., None, :]
    )
    new_n = decay[..., None] * state_n + inflow[..., None] * k_heads
    recalled = jnp.sum(q_heads[..., None] * state_c, axis=2)
    match = jnp.sum(q_heads * k_heads, axis=-1)
    numer = decay[..., None] * recalled + (inflow * match)[..., None] * v_heads
    denom = jnp.maximum(jnp.abs(jnp.sum(q_heads * new_n, axis=-1)), 1.0)
    heads = (numer / denom[..., None]).astype(bf16).reshape(own, -1)
    heads_all = exchange(jnp.broadcast_to(heads[None], (ep_count,) + heads.shape), "ep")
    out_part = jnp.dot(heads_all.reshape(seqs, -1), w_output, preferred_element_type=f32)
    out_part = (out_part + spread.astype(f32) * (1.0 / tp_count)).astype(bf16)
    every = exchange(jnp.broadcast_to(out_part[None], (ep_count * tp_count,) + out_part.shape), BOTH)
    residual = jnp.sum(every.reshape(ep_count, tp_count, seqs, cols).astype(f32), axis=1)
    residual = residual.astype(bf16).transpose(1, 0, 2).reshape(seqs, width)
    normed2 = rms_norm(residual, moe_gain)
    group_count = w_group.shape[1]
    group_prob = jax.nn.softmax(jnp.dot(normed2, w_group, preferred_element_type=f32), axis=-1)
    group_of = (ep_rank * experts_here + jnp.arange(experts_here, dtype=jnp.int32)) // (
        expert_count // group_count
    )
    member = group_of[:, None] == jnp.arange(group_count, dtype=jnp.int32)[None, :]
    chance = jnp.sum(jnp.where(member[None], group_prob[:, None, :], 0.0), axis=-1)
    route = chance * coef
    total = jnp.zeros((seqs, width), f32)
    for x in range(experts_here):
        gate_act = jnp.dot(normed2, w_exp_gate[x], preferred_element_type=f32)
        up_act = jnp.dot(normed2, w_exp_up[x], preferred_element_type=f32)
        hidden = (jax.nn.silu(gate_act) * up_act).astype(bf16)
        total += route[:, x : x + 1] * jnp.dot(hidden, w_exp_down[x], preferred_element_type=f32)
    dense_gate = jax.nn.sigmoid(jnp.dot(normed2, w_dense_gate, preferred_element_type=f32))
    dense_in = lax.dynamic_slice_in_dim(normed2, ep_rank * rows, rows, 1)
    dense = dense_gate[:, None] * jnp.dot(dense_in, w_dense, preferred_element_type=f32)
    total = total.reshape(seqs, tp_count, share)
    mine = jnp.arange(tp_count, dtype=jnp.int32) == tp_rank
    total = (total + jnp.where(mine[None, :, None], dense[:, None, :], 0.0)).astype(bf16)
    total = total.reshape(ep_count, own, tp_count, share).transpose(0, 2, 1, 3)
    last = exchange(total.reshape(ep_count * tp_count, own, share), BOTH)
    own_rows = lax.dynamic_slice(residual, (ep_rank * own, tp_rank * share), (own, share))
    mixed = (own_rows.astype(f32) + jnp.sum(last.astype(f32), axis=0)).astype(bf16)
    return (mixed, new_c, new_n, new_m)


def per_device(*args):
    rows, cols, experts_here = args[5].shape[0], args[11].shape[1], args[16].shape[0]
    seqs = args[0].shape[0] * lax.axis_size("ep")
    fits = (
        lax.axis_size("tp") == 4
        and seqs % 16 == 0
        and rows % 128 == 0
        and cols % 256 == 0
        and experts_here == 1
    )
    return (fast_device if fits else plain_device)(*args)


def solution(mesh):
    placed = (
        P("ep", None),
        P("ep", "tp", None, None),
        P("ep", "tp", None),
        P("ep", "tp"),
        P(),
        P("ep", "tp"),
        P("ep", "tp"),
        P("ep", "tp"),
        P(),
        P(),
        P(),
        P("tp", "ep"),
        P(),
        P(),
        P("ep", None),
        P("ep", None),
        P("ep", None, "tp"),
        P("ep", None, "tp"),
        P("ep", "tp", None),
        P("ep", "tp"),
        P(),
    )
    return jax.shard_map(
        per_device,
        mesh=mesh,
        in_specs=placed,
        out_specs=(P("ep", "tp"), P("ep", "tp", None, None), P("ep", "tp", None), P("ep", "tp")),
        check_vma=False,
    )
```

```python
import functools

import jax
import jax.numpy as jnp
from jax import lax
from jax.experimental import pallas as pl
from jax.experimental.pallas import tpu as pltpu
from jax.sharding import PartitionSpec as P


eps = 1e-06
BOTH = ("ep", "tp")
f32, bf16 = jnp.float32, jnp.bfloat16
VMEM_BYTES = 12 << 20


def exchange(chunks, axes):
    return lax.all_to_all(chunks, axes, split_axis=0, concat_axis=0, tiled=True)


def shaped(*dims, dtype=f32):
    return jax.ShapeDtypeStruct(dims, dtype)


def run(body, outs, scalars, *arrays):
    specs = [pl.BlockSpec(memory_space=pltpu.SMEM)] * len(scalars)
    specs += [pl.BlockSpec(memory_space=pltpu.VMEM)] * len(arrays)
    return pl.pallas_call(
        body,
        out_shape=outs,
        in_specs=specs,
        compiler_params=pltpu.CompilerParams(vmem_limit_bytes=VMEM_BYTES),
    )(*scalars, *arrays)


def dot(left, right, dims=((1,), (0,))):
    return lax.dot_general(left, right, (dims, ((), ())), preferred_element_type=f32)


def gates_body(
    ep_ref, tp_ref,
    tokens_hbm, gain_hbm, in_hbm, forget_hbm, bias_hbm, m_hbm, n_hbm, ids_hbm, weights_hbm,
    query_hbm, key_hbm, value_hbm, moe_gain_hbm, group_hbm, dense_gate_hbm,
    decay_out, inflow_out, new_m_out, kept_n_out, picks_out, joined_out,
    moe_gain_out, group_out, dense_gate_out,
    tokens, gain, w_in, w_forget, bias, state_m, state_n, ids, weights, sems,
):
    small = (
        (tokens_hbm, tokens), (gain_hbm, gain), (in_hbm, w_in), (forget_hbm, w_forget), (bias_hbm, bias),
        (m_hbm, state_m), (n_hbm, state_n), (ids_hbm, ids), (weights_hbm, weights),
    )
    copies = [pltpu.make_async_copy(a, b, sems.at[i]) for i, (a, b) in enumerate(small)]
    at = 0
    for w in (query_hbm, key_hbm, value_hbm):
        place = joined_out.at[:, at : at + w.shape[1]]
        copies.append(pltpu.make_async_copy(w, place, sems.at[len(copies)]))
        at += w.shape[1]
    for a, b in ((moe_gain_hbm, moe_gain_out), (group_hbm, group_out), (dense_gate_hbm, dense_gate_out)):
        copies.append(pltpu.make_async_copy(a, b, sems.at[len(copies)]))
    for copy in copies:
        copy.start()
    for copy in copies[: len(small)]:
        copy.wait()
    own, heads = state_m.shape
    wide = tokens[...].astype(f32)
    inverse = lax.rsqrt(jnp.mean(wide * wide, axis=-1, keepdims=True) + eps)
    normed = (wide * inverse * gain[...]).astype(bf16)
    gate_all = dot(normed, w_in[...], ((1,), (1,)))
    raw = dot(normed, w_forget[...], ((1,), (1,))) + bias[...]
    forget_all = jnp.minimum(raw, 0.0) - jnp.log1p(jnp.exp(-jnp.abs(raw)))
    lane = lax.broadcasted_iota(jnp.int32, gate_all.shape, 1)
    first = tp_ref[0] * heads
    for h in range(heads):
        held = lane == first + h
        in_gate = jnp.sum(jnp.where(held, gate_all, 0.0), axis=1, keepdims=True)
        forget = jnp.sum(jnp.where(held, forget_all, 0.0), axis=1, keepdims=True)
        shifted = forget + state_m[:, h : h + 1]
        new_m = jnp.maximum(shifted, in_gate)
        decay = jnp.exp(shifted - new_m)
        new_m_out[:, h : h + 1] = new_m
        decay_out[:, h : h + 1] = decay
        inflow_out[:, h : h + 1] = jnp.exp(in_gate - new_m)
        for i in range(own):
            kept_n_out[i, h : h + 1, :] = decay[i : i + 1] * state_n[i, h : h + 1, :]
    shares = weights[...] / jnp.sum(weights[...], axis=1, keepdims=True)
    lanes = lax.broadcasted_iota(jnp.int32, (own, picks_out.shape[2]), 1)
    for b in range(picks_out.shape[0]):
        total = jnp.zeros(lanes.shape, f32)
        for j in range(ids.shape[1]):
            here = ids[:, j : j + 1] == b
            total += jnp.where((lanes == 0) & here, shares[:, j : j + 1], 0.0)
        picks_out[b] = total
    for copy in copies[len(small) :]:
        copy.wait()


def norm_body(tokens_hbm, gain_hbm, out, tokens, gain, sems):
    copies = [
        pltpu.make_async_copy(a, b, sems.at[i])
        for i, (a, b) in enumerate(((tokens_hbm, tokens), (gain_hbm, gain)))
    ]
    for copy in copies:
        copy.start()
    for copy in copies:
        copy.wait()
    rows = out.shape[2] // 2
    wide = tokens[...].astype(f32)
    inverse = lax.rsqrt(jnp.mean(wide * wide, axis=-1, keepdims=True) + eps)
    normed = (wide * inverse * gain[...]).astype(bf16)
    for e in range(out.shape[0]):
        out[e, :, :rows] = normed[:, e * rows : (e + 1) * rows]
        out[e, :, rows:] = tokens[:, e * rows : (e + 1) * rows]


def project_body(spread, joined, picks, out):
    own, packed = out.shape[1], joined.shape[1]
    sums = dot(spread[:, : joined.shape[0]], joined[...])
    for b in range(out.shape[0]):
        out[b, :, :packed] = sums[b * own : (b + 1) * own]
        out[b, :, packed:] = picks[b]


def head_columns(values, first, own, head_count, dqk):
    rows = [
        values[i : i + 1, first + h * dqk : first + (h + 1) * dqk]
        for i in range(own)
        for h in range(head_count)
    ]
    rows += [jnp.zeros_like(rows[0])] * (-len(rows) % 8)
    return jnp.transpose(jnp.concatenate(rows, axis=0))


def memory_body(parts, decay, inflow, state_c, kept_n, heads_out, new_n_out, qkv_out, coef_out):
    blocks, own, _ = parts.shape
    head_count, dqk, dv = state_c.shape[1:]
    packed = head_count * (2 * dqk + dv)
    total = parts[0, :, :packed]
    for b in range(1, blocks):
        total += parts[b, :, :packed]
    for b in range(blocks):
        coef_out[b * own : (b + 1) * own, :] = parts[b, :, packed:]
    qkv = total.astype(bf16).astype(f32)
    qkv_out[...] = qkv
    rows = []
    for i in range(own):
        for h in range(head_count):
            q = qkv[i : i + 1, h * dqk : (h + 1) * dqk]
            at = (head_count + h) * dqk
            k = qkv[i : i + 1, at : at + dqk] * dqk ** (-0.5)
            at = 2 * head_count * dqk + h * dv
            v = qkv[i : i + 1, at : at + dv]
            kept, flow = decay[i : i + 1, h : h + 1], inflow[i : i + 1, h : h + 1]
            new_n = kept_n[i, h : h + 1, :] + flow * k
            new_n_out[i, h : h + 1, :] = new_n
            recalled = lax.dot_general(
                q, state_c[i, h], (((1,), (0,)), ((), ())),
                preferred_element_type=f32, precision=lax.Precision.HIGHEST,
            )
            numer = kept * recalled + (flow * jnp.sum(q * k, axis=1, keepdims=True)) * v
            denom = jnp.maximum(jnp.abs(jnp.sum(q * new_n, axis=1, keepdims=True)), 1.0)
            rows.append(numer / denom)
    joined = [jnp.concatenate(rows[i * head_count : (i + 1) * head_count], axis=1) for i in range(own)]
    heads = jnp.concatenate(joined, axis=0).astype(bf16)
    for d in range(heads_out.shape[0]):
        heads_out[d] = heads


def output_body(tp_ref, heads, near, side_near, far, side_far, spread, out):
    own = heads.shape[1]
    tp_count = heads.shape[0] * own // spread.shape[0]
    half, some = out.shape[2], out.shape[1]
    rank = tp_ref[0]
    side, part = rank % 2, rank // 2
    blocks = some // own
    at = pl.ds(pl.multiple_of(side * half, 128), half)
    rows = spread.shape[1] // 2
    tokens = spread[:, pl.ds(pl.multiple_of(rows + side * half, 128), half)].astype(f32)
    total = jnp.zeros((some, half), f32)
    for d in range(tp_count):
        source = rank ^ d
        pieces = [heads[(part * blocks + b) * tp_count + source].astype(f32) for b in range(blocks)]
        left = jnp.concatenate(pieces, axis=0).astype(bf16)
        total += dot(left, (near, side_near, far, side_far)[d][:, at]).astype(bf16).astype(f32)
    total = (total + jnp.where(part == 0, tokens[:some], tokens[some:])).astype(bf16)
    for d in range(out.shape[0]):
        out[d] = total


def experts_body(
    ep_ref, tp_ref, every, coef, gain, w_group, w_dense_gate, w_gate, w_up, w_down, w_dense,
    qkv, decay, inflow, state_c, new_n, new_m,
    out, own_out, new_c_out, new_n_out, new_m_out, scaled_buf, total_buf, new_c, sems,
    *, per_group, ep_count,
):
    saved = [
        pltpu.make_async_copy(a, b, sems.at[i])
        for i, (a, b) in enumerate(((new_n, new_n_out), (new_m, new_m_out), (new_c, new_c_out)))
    ]
    saved[0].start()
    saved[1].start()
    seqs, _ = scaled_buf.shape
    count, _, _ = every.shape
    tp_count = count // ep_count
    own, share = out.shape[1], out.shape[2]
    ep_rank, tp_rank = ep_ref[0], tp_ref[0]
    halves = []
    for part in range(2):
        tiles = [every[e * tp_count + part * 2 + s].astype(f32) for e in range(ep_count) for s in range(2)]
        halves.append(jnp.concatenate(tiles, axis=1))
    residual = jnp.concatenate(halves, axis=0)
    inverse = lax.rsqrt(jnp.mean(residual * residual, axis=-1, keepdims=True) + eps)
    narrow = (residual * inverse * gain[...]).astype(bf16)
    scaled_buf[...] = narrow.astype(f32)
    total_buf[...] = residual
    logits = dot(narrow, w_group[...], ((1,), (1,)))
    gate_act = dot(narrow, w_gate[0])
    up_act = dot(narrow, w_up[0])
    rows = w_dense.shape[0]
    some_in = scaled_buf[:, pl.ds(pl.multiple_of(ep_rank * rows, 128), rows)].astype(bf16)
    dense = dot(some_in, w_dense[...])
    held_seqs, head_count, dqk, dv = state_c.shape
    turned = head_columns(qkv[...], head_count * dqk, held_seqs, head_count, dqk)
    for i in range(held_seqs):
        for h in range(head_count):
            at = 2 * head_count * dqk + h * dv
            flow = inflow[i : i + 1, h : h + 1] * dqk ** (-0.5)
            column = turned[:, i * head_count + h : i * head_count + h + 1]
            fresh = column * (flow * qkv[i : i + 1, at : at + dv])
            new_c[i, h] = decay[i : i + 1, h : h + 1] * state_c[i, h] + fresh
    saved[2].start()
    hidden = (gate_act * jax.nn.sigmoid(gate_act) * up_act).astype(bf16)
    down = dot(hidden, w_down[0])
    powers = jnp.exp(logits - jnp.max(logits, axis=1, keepdims=True))
    lane = lax.broadcasted_iota(jnp.int32, logits.shape, 1)
    chosen = jnp.sum(jnp.where(lane == ep_rank // per_group, powers, 0.0), axis=1, keepdims=True)
    route = chosen / jnp.sum(powers, axis=1, keepdims=True) * coef[:, 0:1]
    vector = w_dense_gate[...].astype(f32)
    lanes = vector.shape[1]
    gate = jnp.zeros((seqs, lanes), f32)
    for r in range(vector.shape[0]):
        gate += narrow[:, r * lanes : (r + 1) * lanes].astype(f32) * vector[r : r + 1, :]
    gate = jnp.sum(gate, axis=1, keepdims=True)
    columns = pl.ds(pl.multiple_of(tp_rank * share, 128), share)
    mine = total_buf[:, columns]
    row = lax.broadcasted_iota(jnp.int32, mine.shape, 0)
    for i in range(own):
        held = jnp.where(row == ep_rank * own + i, mine, 0.0)
        own_out[i : i + 1, :] = jnp.sum(held, axis=0, keepdims=True)
    total_buf[...] = route * down
    total_buf[:, columns] += jax.nn.sigmoid(gate) * dense
    for b in range(ep_count):
        for t in range(tp_count):
            piece = total_buf[b * own : (b + 1) * own, t * share : (t + 1) * share]
            out[b * tp_count + t] = piece.astype(bf16)
    for copy in saved:
        copy.wait()


def fast_device(*args):
    return fast_rounds(*args)


def fast_rounds(
    tokens, state_c, state_n, state_m, mix_gain, w_query, w_key, w_value, w_input_gate, w_forget_gate,
    forget_bias, w_output, moe_gain, w_group, expert_ids, expert_weight, w_exp_gate, w_exp_up,
    w_exp_down, w_dense, w_dense_gate,
):
    own, width = tokens.shape
    tp_count, ep_count = lax.axis_size("tp"), lax.axis_size("ep")
    tp_rank, ep_rank = lax.axis_index("tp"), lax.axis_index("ep")
    every_count = ep_count * tp_count
    seqs, (rows, qk_cols), v_cols = own * ep_count, w_query.shape, w_value.shape[1]
    head_count, share, half = state_m.shape[1], width // tp_count, w_output.shape[1] // 2
    tp_ref, ep_ref = tp_rank.reshape(1), ep_rank.reshape(1)
    gain = mix_gain.reshape(1, width)
    packed = 2 * qk_cols + v_cols
    chunks = pl.pallas_call(
        norm_body,
        out_shape=shaped(ep_count, own, 2 * rows, dtype=bf16),
        in_specs=[pl.BlockSpec(memory_space=pltpu.HBM)] * 2,
        scratch_shapes=[pltpu.VMEM(a.shape, a.dtype) for a in (tokens, gain)]
        + [pltpu.SemaphoreType.DMA((2,))],
        name="norm",
        compiler_params=pltpu.CompilerParams(vmem_limit_bytes=VMEM_BYTES),
    )(*[pltpu.with_memory_space_constraint(a, pltpu.HBM) for a in (tokens, gain)])
    spread = exchange(chunks, "ep")
    spread = spread.reshape(seqs, 2 * rows)
    swapped = [(d, d ^ 1) for d in range(tp_count)]
    far = lax.ppermute(w_output, "tp", [(d, d ^ 2) for d in range(tp_count)])
    sources = (
        tokens, gain, w_input_gate.T, w_forget_gate.T, forget_bias.reshape(1, -1), state_m, state_n,
        expert_ids, expert_weight,
    )
    later = (moe_gain.reshape(1, width), w_group.T, w_dense_gate.reshape(-1, 128))
    decay, inflow, new_m, kept_n, picks, joined, *later_held = pl.pallas_call(
        gates_body,
        out_shape=(shaped(own, head_count),) * 3
        + (shaped(*state_n.shape), shaped(ep_count, own, 128))
        + (shaped(rows, packed, dtype=bf16),)
        + tuple(shaped(*a.shape, dtype=a.dtype) for a in later),
        in_specs=[pl.BlockSpec(memory_space=pltpu.SMEM)] * 2 + [pl.BlockSpec(memory_space=pltpu.HBM)] * 15,
        scratch_shapes=[pltpu.VMEM(a.shape, a.dtype) for a in sources]
        + [pltpu.SemaphoreType.DMA((len(sources) + 6,))],
        name="gates",
        compiler_params=pltpu.CompilerParams(vmem_limit_bytes=VMEM_BYTES),
    )(ep_ref, tp_ref, *[pltpu.with_memory_space_constraint(a, pltpu.HBM) for a in (*sources, w_query, w_key, w_value, *later)])
    side_near = lax.ppermute(w_output, "tp", swapped)
    sums = run(
        project_body, shaped(ep_count, own, packed + 128), (),
        spread, joined, picks,
    )
    parts = exchange(sums, "ep")
    parts, far, side_near = lax.optimization_barrier((parts, far, side_near))
    side_far = lax.ppermute(far, "tp", swapped)
    heads, new_n, qkv, coef = run(
        memory_body,
        (
            shaped(every_count, own, v_cols, dtype=bf16), shaped(*state_n.shape),
            shaped(own, packed), shaped(seqs, 128),
        ),
        (), parts, decay, inflow, state_c, kept_n,
    )
    heads = exchange(heads, BOTH)
    out = run(
        output_body, shaped(every_count, seqs // 2, half, dtype=bf16), (tp_ref,),
        heads, w_output, side_near, far, side_far, spread,
    )
    every = exchange(out, BOTH)
    last, own_rows, new_c, new_n, new_m = pl.pallas_call(
        functools.partial(
            experts_body, per_group=ep_count // w_group.shape[1], ep_count=ep_count
        ),
        out_shape=(
            shaped(every_count, own, share, dtype=bf16), shaped(own, share),
            shaped(*state_c.shape), shaped(*state_n.shape), shaped(*state_m.shape),
        ),
        in_specs=[pl.BlockSpec(memory_space=pltpu.SMEM)] * 2 + [pl.BlockSpec(memory_space=pltpu.VMEM)] * 15,
        out_specs=[pl.BlockSpec(memory_space=pltpu.VMEM)] * 2 + [pl.BlockSpec(memory_space=pltpu.HBM)] * 3,
        scratch_shapes=[pltpu.VMEM((seqs, width), f32)] * 2
        + [pltpu.VMEM(state_c.shape, f32), pltpu.SemaphoreType.DMA((3,))],
        name="experts",
        compiler_params=pltpu.CompilerParams(vmem_limit_bytes=VMEM_BYTES),
    )(
        ep_ref, tp_ref, every, coef, *later_held,
        w_exp_gate, w_exp_up, w_exp_down, w_dense, qkv, decay, inflow, state_c,
        new_n, new_m,
    )
    last = exchange(last, BOTH)
    mixed = (own_rows + jnp.sum(last.astype(f32), axis=0)).astype(bf16)
    return (mixed, new_c, new_n, new_m)


def rms_norm(values, gain):
    widened = values.astype(jnp.float32)
    inverse = lax.rsqrt(jnp.mean(widened * widened, axis=-1, keepdims=True) + eps)
    return (widened * inverse * gain).astype(jnp.bfloat16)


def plain_device(
    tokens,
    state_c,
    state_n,
    state_m,
    mix_gain,
    w_query,
    w_key,
    w_value,
    w_input_gate,
    w_forget_gate,
    forget_bias,
    w_output,
    moe_gain,
    w_group,
    expert_ids,
    expert_weight,
    w_exp_gate,
    w_exp_up,
    w_exp_down,
    w_dense,
    w_dense_gate,
):
    own, width = tokens.shape
    tp_count = lax.axis_size("tp")
    ep_count = lax.axis_size("ep")
    tp_rank = lax.axis_index("tp")
    ep_rank = lax.axis_index("ep")
    seqs = own * ep_count
    head_count = state_m.shape[1]
    rows = w_query.shape[0]
    qk_cols = w_query.shape[1]
    share = width // tp_count
    cols = w_output.shape[1]
    experts_here = w_exp_gate.shape[0]
    expert_count = experts_here * ep_count

    spread = exchange(tokens.reshape(own, ep_count, rows).transpose(1, 0, 2), "ep")
    spread = spread.reshape(seqs, rows)
    gain_rows = lax.dynamic_slice_in_dim(mix_gain, ep_rank * rows, rows)
    scaled = (spread.astype(f32) * gain_rows).astype(bf16)
    sums = [jnp.dot(scaled, w, preferred_element_type=f32) for w in (w_query, w_key, w_value)]
    expert_of = jnp.arange(expert_count, dtype=jnp.int32)
    shares = expert_weight / jnp.sum(expert_weight, axis=1, keepdims=True)
    picks = jnp.sum(
        jnp.where(expert_ids[None, :, :] == expert_of[:, None, None], shares[None], 0.0), axis=2
    )
    picks = picks.reshape(ep_count, experts_here, own).transpose(0, 2, 1)
    picks = jnp.pad(picks, ((0, 0), (0, 0), (0, -experts_here % 128))).reshape(seqs, -1)
    parts = exchange(jnp.concatenate(sums + [picks], axis=1).reshape(ep_count, own, -1), "ep")
    wide = tokens.astype(f32)
    inverse = lax.rsqrt(jnp.mean(wide * wide, axis=-1, keepdims=True) + eps)
    normed = (wide * inverse * mix_gain).astype(bf16)
    packed = 2 * qk_cols + w_value.shape[1]
    coef = parts[:, :, packed : packed + experts_here].reshape(seqs, experts_here)
    qkv = (jnp.sum(parts[:, :, :packed], axis=0) * inverse).astype(bf16).astype(f32)
    gate_all = jnp.dot(normed, w_input_gate, preferred_element_type=f32)
    forget_all = jax.nn.log_sigmoid(
        jnp.dot(normed, w_forget_gate, preferred_element_type=f32) + forget_bias
    )
    in_gate = lax.dynamic_slice_in_dim(gate_all, tp_rank * head_count, head_count, 1)
    forget = lax.dynamic_slice_in_dim(forget_all, tp_rank * head_count, head_count, 1)
    q_heads = qkv[:, :qk_cols].reshape(own, head_count, -1)
    k_heads = qkv[:, qk_cols : 2 * qk_cols].reshape(own, head_count, -1)
    k_heads = k_heads * q_heads.shape[-1] ** (-0.5)
    v_heads = qkv[:, 2 * qk_cols :].reshape(own, head_count, -1)
    new_m = jnp.maximum(forget + state_m, in_gate)
    decay = jnp.exp(forget + state_m - new_m)
    inflow = jnp.exp(in_gate - new_m)
    new_c = (
        decay[..., None, None] * state_c
        + (inflow[..., None] * k_heads)[..., :, None] * v_heads[..., None, :]
    )
    new_n = decay[..., None] * state_n + inflow[..., None] * k_heads
    recalled = jnp.sum(q_heads[..., None] * state_c, axis=2)
    match = jnp.sum(q_heads * k_heads, axis=-1)
    numer = decay[..., None] * recalled + (inflow * match)[..., None] * v_heads
    denom = jnp.maximum(jnp.abs(jnp.sum(q_heads * new_n, axis=-1)), 1.0)
    heads = (numer / denom[..., None]).astype(bf16).reshape(own, -1)
    heads_all = exchange(jnp.broadcast_to(heads[None], (ep_count,) + heads.shape), "ep")
    out_part = jnp.dot(heads_all.reshape(seqs, -1), w_output, preferred_element_type=f32)
    out_part = (out_part + spread.astype(f32) * (1.0 / tp_count)).astype(bf16)
    every = exchange(jnp.broadcast_to(out_part[None], (ep_count * tp_count,) + out_part.shape), BOTH)
    residual = jnp.sum(every.reshape(ep_count, tp_count, seqs, cols).astype(f32), axis=1)
    residual = residual.astype(bf16).transpose(1, 0, 2).reshape(seqs, width)
    normed2 = rms_norm(residual, moe_gain)
    group_count = w_group.shape[1]
    group_prob = jax.nn.softmax(jnp.dot(normed2, w_group, preferred_element_type=f32), axis=-1)
    group_of = (ep_rank * experts_here + jnp.arange(experts_here, dtype=jnp.int32)) // (
        expert_count // group_count
    )
    member = group_of[:, None] == jnp.arange(group_count, dtype=jnp.int32)[None, :]
    chance = jnp.sum(jnp.where(member[None], group_prob[:, None, :], 0.0), axis=-1)
    route = chance * coef
    total = jnp.zeros((seqs, width), f32)
    for x in range(experts_here):
        gate_act = jnp.dot(normed2, w_exp_gate[x], preferred_element_type=f32)
        up_act = jnp.dot(normed2, w_exp_up[x], preferred_element_type=f32)
        hidden = (jax.nn.silu(gate_act) * up_act).astype(bf16)
        total += route[:, x : x + 1] * jnp.dot(hidden, w_exp_down[x], preferred_element_type=f32)
    dense_gate = jax.nn.sigmoid(jnp.dot(normed2, w_dense_gate, preferred_element_type=f32))
    dense_in = lax.dynamic_slice_in_dim(normed2, ep_rank * rows, rows, 1)
    dense = dense_gate[:, None] * jnp.dot(dense_in, w_dense, preferred_element_type=f32)
    total = total.reshape(seqs, tp_count, share)
    mine = jnp.arange(tp_count, dtype=jnp.int32) == tp_rank
    total = (total + jnp.where(mine[None, :, None], dense[:, None, :], 0.0)).astype(bf16)
    total = total.reshape(ep_count, own, tp_count, share).transpose(0, 2, 1, 3)
    last = exchange(total.reshape(ep_count * tp_count, own, share), BOTH)
    own_rows = lax.dynamic_slice(residual, (ep_rank * own, tp_rank * share), (own, share))
    mixed = (own_rows.astype(f32) + jnp.sum(last.astype(f32), axis=0)).astype(bf16)
    return (mixed, new_c, new_n, new_m)


def per_device(*args):
    rows, cols, experts_here = args[5].shape[0], args[11].shape[1], args[16].shape[0]
    seqs = args[0].shape[0] * lax.axis_size("ep")
    fits = (
        lax.axis_size("tp") == 4
        and seqs % 16 == 0
        and rows % 128 == 0
        and cols % 256 == 0
        and experts_here == 1
    )
    return (fast_device if fits else plain_device)(*args)


def solution(mesh):
    placed = (
        P("ep", None),
        P("ep", "tp", None, None),
        P("ep", "tp", None),
        P("ep", "tp"),
        P(),
        P("ep", "tp"),
        P("ep", "tp"),
        P("ep", "tp"),
        P(),
        P(),
        P(),
        P("tp", "ep"),
        P(),
        P(),
        P("ep", None),
        P("ep", None),
        P("ep", None, "tp"),
        P("ep", None, "tp"),
        P("ep", "tp", None),
        P("ep", "tp"),
        P(),
    )
    return jax.shard_map(
        per_device,
        mesh=mesh,
        in_specs=placed,
        out_specs=(P("ep", "tp"), P("ep", "tp", None, None), P("ep", "tp", None), P("ep", "tp")),
        check_vma=False,
    )
```
